32 devices in a mesh: sp: 8 (over z, x), tp: 4 (over y, core).
Axes of the slice: x: 2, y: 2, z: 4, core: 2. Of those that a mesh axis runs over, the one named last changes fastest.
Arguments:
- activations: bfloat16 [4096, 1024], P(('sp', 'tp')), may hold values from -8 to 8, as said below
- input_gain: float32 [1024], replicated, may hold values from 0.5 to 1.5
- query_weight: bfloat16 [1024, 1024], P(None, 'tp'), may hold values from -0.1875 to 0.1875
- key_weight: bfloat16 [1024, 1024], P(None, 'tp'), may hold values from -0.375 to 0.375
- value_weight: bfloat16 [1024, 1024], P(None, 'tp'), may hold values from -0.1875 to 0.1875
- stop_offset: float32 [16], P('tp'), may hold values from -16 to 0, as said below
- output_weight: bfloat16 [1024, 1024], P('tp'), may hold values from -0.1875 to 0.1875
- output_gain: float32 [1024], replicated, may hold values from 0.5 to 1.5
Outputs:
- layer_out: bfloat16 [4096, 1024], P(('sp', 'tp'))
The draws below stay inside these ranges and needn't reach their ends.
Inputs may be any that keep to these rules, and one draw needn't show every extreme that they name: activations are noise of about unit size plus a mean vector of about unit size shared by each aligned block of 512 rows and different between runs; each row as a whole may also be scaled by a factor between 0.25 and 2; the result is clipped to the range. `stop_offset`: each entry equals minus the natural logarithm of 4096, minus 2, plus the natural logarithm of 3, plus a number between 0 and 0.7.
All inputs are finite; a program needn't handle non-finite values.
Results may differ from the reference program's by a relative error of at most 0.015.
Values may be sent and summed in bfloat16 or wider, within the bound.
A program may use at most 128 MiB of HBM per device.

```python
import jax
import jax.numpy as jnp
from jax import lax

D = 1024
HEADS = 16
HEAD_DIM = 64
TOK_DEV = 512
TOKENS = 4096


def draw_activations(key, part):
    noise_key, mean_key, scale_key = jax.random.split(key, 3)
    blocks = TOKENS // TOK_DEV
    noise_part = jax.random.normal(noise_key, (blocks, TOK_DEV, D), jnp.float32)
    block_means = jax.random.normal(mean_key, (blocks, 1, D), jnp.float32)
    combined = noise_part + block_means
    return jnp.clip(combined, -8.0, 8.0).reshape(TOKENS, D).astype(jnp.bfloat16)


def draw_stop_offset(key, part):
    center = -jnp.log(jnp.float32(TOKENS)) - 2.0 + jnp.log(jnp.float32(3.0))
    return center + jax.random.uniform(key, (HEADS,), jnp.float32, 0.0, 0.7)


def steps_of(own_key, dims, cuts, least, top_value):
    loudness, own = 1.0, jax.random.fold_in(own_key, 6)
    for position, parts in cuts:
        draws = jnp.exp(jax.random.uniform(jax.random.fold_in(own, position), (parts,), jnp.float32, least / len(cuts), top_value / len(cuts)))
        loudness = loudness * jnp.repeat(draws, dims[position] // parts).reshape([-1 if axis == position else 1 for axis in range(len(dims))])
    return loudness


def centred(rng, dims, width, most, cuts=(), kind=jnp.bfloat16):
    level = steps_of(rng, dims, cuts, -0.22, 0.18) if cuts else 1.0
    drawn = jax.random.normal(rng, dims, jnp.float32) * width * level
    return jnp.minimum(jnp.maximum(drawn, -most), most).astype(kind)


def setup_inputs(seed: int = 0) -> dict:
    arg_keys = jax.random.split(jax.random.key(seed), 9)
    return {
        "activations": draw_activations(jax.random.fold_in(arg_keys[8], 71), 0),
        "input_gain": jnp.clip(1.0 + 0.1 * jax.random.normal(arg_keys[1], (D,), jnp.float32), 0.5, 1.5),
        "query_weight": centred(arg_keys[2], (D, HEADS * HEAD_DIM), D ** -0.5, 0.1875, ((1, 4),)),
        "key_weight": centred(arg_keys[3], (D, HEADS * HEAD_DIM), (D // 4) ** -0.5, 0.375, ((1, 4),)),
        "value_weight": centred(arg_keys[4], (D, HEADS * HEAD_DIM), D ** -0.5, 0.1875, ((1, 4),)),
        "stop_offset": draw_stop_offset(jax.random.fold_in(arg_keys[8], 71), 0),
        "output_weight": centred(arg_keys[6], (HEADS * HEAD_DIM, D), (HEADS * HEAD_DIM) ** -0.5, 0.1875, ((0, 4),)),
        "output_gain": jnp.clip(1.0 + 0.1 * jax.random.normal(arg_keys[7], (D,), jnp.float32), 0.5, 1.5),
    }


epsilon = 1e-06

def scaled_rows(row_block, row_gain):
    widened = row_block.astype(jnp.float32)
    spread = lax.optimization_barrier(jnp.mean(widened * widened, axis=-1, keepdims=True))
    return (widened * lax.rsqrt(spread + epsilon) * row_gain).astype(jnp.bfloat16)

def reference(activations, input_gain, query_weight, key_weight, value_weight, stop_offset, output_weight, output_gain):
    normed = scaled_rows(activations, input_gain)
    query_rows = jnp.dot(normed, query_weight, preferred_element_type=jnp.float32).astype(jnp.bfloat16)
    key_rows = jnp.dot(normed, key_weight, preferred_element_type=jnp.float32).astype(jnp.bfloat16)
    value_rows = jnp.dot(normed, value_weight, preferred_element_type=jnp.float32).astype(jnp.bfloat16)
    blocks = TOKENS // TOK_DEV
    query_blocks = query_rows.reshape(blocks, TOK_DEV, HEADS, HEAD_DIM)
    key_blocks = key_rows.reshape(blocks, TOK_DEV, HEADS, HEAD_DIM)
    value_blocks = value_rows.reshape(blocks, TOK_DEV, HEADS, HEAD_DIM)
    score_scale = HEAD_DIM ** (-0.5)
    offsets = stop_offset.astype(jnp.float32)

    def attend_block(query_index):
        queries = query_blocks[query_index].astype(jnp.float32)
        first_query = query_index * TOK_DEV

        def per_key(key_index):

            def compute(unused):
                key_here = key_blocks[key_index].astype(jnp.float32)
                value_here = value_blocks[key_index].astype(jnp.float32)
                scores = jnp.einsum('thd,shd->hts', queries, key_here, precision=lax.Precision.HIGHEST)
                scores = scores * score_scale + offsets[:, None, None]
                query_pos = first_query + jnp.arange(TOK_DEV, dtype=jnp.int32)
                key_pos = key_index * TOK_DEV + jnp.arange(TOK_DEV, dtype=jnp.int32)
                earlier = key_pos[None, :] < query_pos[:, None]
                log_keep = jnp.where(earlier[None], jax.nn.log_sigmoid(-scores), 0.0)
                within = lax.cumsum(log_keep, axis=2, reverse=True) - log_keep
                weights = jnp.where(earlier[None], jnp.exp(jax.nn.log_sigmoid(scores) + within), 0.0)
                weights = weights.astype(jnp.bfloat16).astype(jnp.float32)
                shard_part = jnp.einsum('hts,shd->thd', weights, value_here, precision=lax.Precision.HIGHEST)
                return (shard_part, lax.optimization_barrier(jnp.sum(log_keep, axis=2)))

            def skipped(unused):
                return (jnp.zeros((TOK_DEV, HEADS, HEAD_DIM), jnp.float32), jnp.zeros((HEADS, TOK_DEV), jnp.float32))
            return lax.cond(key_index <= query_index, compute, skipped, 0)
        block_parts, totals = lax.map(per_key, jnp.arange(blocks, dtype=jnp.int32))
        prefix_sums = jnp.cumsum(totals, axis=0)
        factors = jnp.exp(prefix_sums[-1:] - prefix_sums)
        combined = jnp.einsum('bht,bthd->thd', factors, block_parts, precision=lax.Precision.HIGHEST)
        return combined.astype(jnp.bfloat16)
    attended = lax.map(attend_block, jnp.arange(blocks, dtype=jnp.int32))
    attended = attended.reshape(TOKENS, HEADS * HEAD_DIM)
    projected = jnp.dot(attended, output_weight, preferred_element_type=jnp.float32)
    return scaled_rows(projected, output_gain)
```

```python
import functools

import jax
import jax.numpy as jnp
from jax import lax
from jax.experimental import pallas as pl
from jax.experimental.pallas import tpu as pltpu
from jax.sharding import PartitionSpec as P

epsilon = 1e-06
log2e = 1.4426950408889634
MESH = pl.DeviceIdType.MESH
f32 = jnp.float32
bf16 = jnp.bfloat16


def scaled_rows(widened, row_gain):
    spread = jnp.mean(widened * widened, axis=-1, keepdims=True)
    return (widened * lax.rsqrt(spread + epsilon) * row_gain).astype(bf16)


def layer_kernel(
    S,
    T,
    H,
    dh,
    act,
    gain_in,
    wq,
    wk,
    wv,
    off,
    wo,
    gain_out,
    out,
    xg,
    wg,
    kvs,
    qs,
    kv,
    qr,
    qpad,
    tri,
    acc,
    carry,
    obuf,
    orecv,
    att,
    x_send,
    x_recv,
    w_send,
    w_recv,
    kv_send,
    kv_relay,
    kv_recv,
    q_send,
    q_recv,
    o_send,
    o_recv,
):
    G = S // H
    R = act.shape[0]
    B = R * T
    half = B // 2
    rows = wo.shape[0]
    s = lax.axis_index("sp")
    t = lax.axis_index("tp")
    h, g = s // G, s % G
    y, c = t // 2, t % 2
    partner = y * 2 + 1 - c
    Y = T // 2

    def owner(group):
        turn = s % (2 * G) if group is None else None
        return jnp.where(turn < G, turn, 2 * G - 1 - turn)

    gq = owner(None)

    def block_of(k):
        return k * G + (g if k % 2 == 0 else G - 1 - g)

    def remote(src, dst, send, recv, dev):
        return pltpu.make_async_remote_copy(
            src_ref=src, dst_ref=dst, send_sem=send, recv_sem=recv, device_id=dev, device_id_type=MESH
        )

    started = []

    def go(copy):
        copy.start()
        started.append(copy)
        return copy

    def xrow(index):
        return xg.at[pl.ds(pl.multiple_of(index * R, R), R)]

    def wrow(index):
        return wg.at[pl.ds(pl.multiple_of(index * rows, rows), rows)]

    def x_copy(index, slot, dev):
        return remote(xrow(index), xrow(index), x_send.at[slot], x_recv.at[index], (s, dev))

    def w_copy(src, index, slot, dev):
        return remote(src, wrow(index), w_send.at[slot], w_recv.at[index], (s, dev))

    xg[pl.ds(pl.multiple_of(t * R, R), R)] = scaled_rows(act[...].astype(f32), gain_in[...])
    for e in range(1, Y):
        go(x_copy(t, e, ((y + e) % Y) * 2 + c))
    go(x_copy(t, 0, partner))
    wg[pl.ds(pl.multiple_of(t * rows, rows), rows)] = wo[...]
    high = lax.broadcasted_iota(jnp.int32, (B, half), 0)
    low = lax.broadcasted_iota(jnp.int32, (B, half), 1)
    tri[...] = (high > low).astype(f32).astype(bf16)
    for e in range(1, Y):
        came = ((y + e) % Y) * 2 + c
        x_copy(came, 0, partner).wait_recv()
        go(x_copy(came, Y + e - 1, partner))
    for e in range(1, Y):
        go(w_copy(wo, t, e, ((y + e) % Y) * 2 + c))
    x_copy(partner, 0, partner).wait_recv()
    for e in range(1, Y):
        x_copy(((y + e) % Y) * 2 + 1 - c, 0, partner).wait_recv()

    rows_all = xg[...]
    keys = jnp.dot(rows_all, wk[...], preferred_element_type=f32).astype(bf16)
    values = jnp.dot(rows_all, wv[...], preferred_element_type=f32).astype(bf16)
    for i in range(H):
        cols = slice(i * dh, (i + 1) * dh)
        kvs[i] = jnp.concatenate([keys[:, cols], values[:, cols]], axis=1)
    kv_copies = []
    for d in range(1, H):
        hd = (h + d) % H
        go(remote(kvs.at[hd], kv.at[s], kv_send.at[d], kv_recv.at[s], (hd * G + g, t)))
    for e in range(1, G):
        go(remote(kvs.at[h], kv.at[s], kv_relay.at[e - 1], kv_recv.at[s], (h * G + (g + e) % G, t)))
    kv[s] = kvs[h]
    queries = jnp.dot(rows_all, wq[...], preferred_element_type=f32).astype(bf16)
    for i in range(H):
        cols = slice(i * dh, (i + 1) * dh)
        qs[i] = jnp.concatenate([queries[:half, cols], queries[half:, cols]], axis=1)
    for d in range(1, H):
        hd = (h + d) % H
        go(remote(qs.at[hd], qr.at[s // G], q_send.at[d], q_recv.at[s // G], (hd * G + gq, t)))

    own_q = remote(qs.at[h], qr.at[s // G], q_send.at[0], q_recv.at[s // G], (h * G + gq, t))

    @pl.when(gq != g)
    def _():
        own_q.start()

    @pl.when(gq == g)
    def _():
        qr[s // G] = qs[h]

    def kv_wait(j):
        remote(kvs.at[0], kv.at[j], kv_send.at[0], kv_recv.at[j], (s, t)).wait_recv()

    go(w_copy(wo, t, 0, partner))
    for e in range(1, Y):
        came = ((y + e) % Y) * 2 + c
        w_copy(wo, came, 0, partner).wait_recv()
        go(w_copy(wrow(came), came, Y + e - 1, partner))

    for d in range(1, H):
        hd = (h + d) % H
        j = hd * G + g
        kv_wait(j)
        for e in range(1, G):
            go(
                remote(
                    kv.at[j],
                    kv.at[j],
                    kv_relay.at[d * (G - 1) + e - 1],
                    kv_recv.at[j],
                    (h * G + (g + e) % G, t),
                )
            )

    offset = off[h] * log2e
    factor = dh ** (-0.5) * log2e

    def piece(i, block, width, causal):
        key_tile = kv[block, :width]
        z = lax.dot_general(qpad[i], key_tile, (((1,), (1,)), ((), ())), preferred_element_type=f32)
        z = z * factor + offset
        keep = jnp.maximum(jnp.log2(1.0 + jnp.exp2(jnp.minimum(z, 100.0))), z)
        if causal:
            query_pos = i * half + lax.broadcasted_iota(jnp.int32, (half, width), 0)
            earlier = lax.broadcasted_iota(jnp.int32, (half, width), 1) < query_pos
            lost = jnp.where(earlier, keep, 0.0)
        else:
            lost = keep
        lost_b = lost.astype(bf16)
        first = jnp.dot(lost_b, tri[:width], preferred_element_type=f32)
        after = first
        if width > half:
            last = jnp.dot(lost_b[:, half:], tri[:half], preferred_element_type=f32)
            after = jnp.concatenate([first, last], axis=1)
        weight = jnp.exp2(z - keep - after)
        if causal:
            weight = jnp.where(earlier, weight, 0.0)
        part = jnp.dot(weight.astype(bf16), key_tile, preferred_element_type=f32)
        total = first[:, :1] + lost[:, :1]
        if causal:
            acc[i] = part
            carry[i] = jnp.broadcast_to(total, carry.shape[1:])
        else:
            before = carry[i]
            acc[i] += jnp.exp2(-before) * part
            carry[i] = before + total

    for k in range(H):
        b = block_of(k)
        for e in range(1, G):
            kv_wait(k * G + (g + e) % G)

        @pl.when(b != s)
        def _():
            remote(qs.at[0], qr.at[k], q_send.at[0], q_recv.at[k], (s, t)).wait_recv()

        packed = qr[k]
        blank = jnp.zeros((half, dh), bf16)
        qpad[0] = jnp.concatenate([packed[:, :dh], blank], axis=1)
        qpad[1] = jnp.concatenate([packed[:, dh:], blank], axis=1)
        piece(0, b, half, True)
        piece(1, b, B, True)

        def more(step, unused):
            piece(0, b - 1 - step, B, False)
            piece(1, b - 1 - step, B, False)
            return unused

        lax.fori_loop(0, b, more, 0)
        per = max(half // R, 1)
        for r in range(T):
            chunk = acc[r * R // half, pl.ds(r * R % half, R)]
            obuf[k, r] = jnp.concatenate([chunk[: R // 2, dh:], chunk[R // 2 :, dh:]], axis=1).astype(bf16)
        for e in range(1, T):
            r = (t + e) % T
            go(remote(obuf.at[k, r], orecv.at[t * H + h], o_send.at[k * T + e], o_recv.at[t * H + h], (b, r)))
        own_o = remote(obuf.at[k, t], orecv.at[t * H + h], o_send.at[k * T], o_recv.at[t * H + h], (b, t))

        @pl.when(b != s)
        def _():
            own_o.start()

        @pl.when(b == s)
        def _():
            orecv[t * H + h] = obuf[k, t]

    w_copy(wo, partner, 0, partner).wait_recv()
    for e in range(1, Y):
        w_copy(wo, ((y + e) % Y) * 2 + 1 - c, 0, partner).wait_recv()

    for tt in range(T):
        for hh in range(H):

            @pl.when(jnp.logical_or(tt != t, hh * G + gq != s))
            def _():
                e = tt * H + hh
                remote(obuf.at[0, 0], orecv.at[e], o_send.at[0], o_recv.at[e], (s, t)).wait_recv()

    for p in range(T * H // 2):
        one, two = orecv[2 * p], orecv[2 * p + 1]
        cols = slice(2 * p * dh, (2 * p + 2) * dh)
        att[: R // 2, cols] = jnp.concatenate([one[:, :dh], two[:, :dh]], axis=1)
        att[R // 2 :, cols] = jnp.concatenate([one[:, dh:], two[:, dh:]], axis=1)
    projected = jnp.dot(att[...], wg[...], preferred_element_type=f32)
    out[...] = scaled_rows(projected, gain_out[...])

    for copy in started:
        copy.wait_send()

    @pl.when(gq != g)
    def _():
        own_q.wait_send()

    for k in range(H):
        b = block_of(k)

        @pl.when(b != s)
        def _():
            remote(obuf.at[k, t], orecv.at[t * H + h], o_send.at[k * T], o_recv.at[t * H + h], (b, t)).wait_send()


def solution(mesh):
    S, T = mesh.shape["sp"], mesh.shape["tp"]

    def local(act, gain_in, wq, wk, wv, off, wo, gain_out):
        R, D = act.shape
        H = off.shape[0]
        dh = wq.shape[1] // H
        G = S // H
        B = R * T
        half = B // 2
        vmem = pl.BlockSpec(memory_space=pltpu.VMEM)
        smem = pl.BlockSpec(memory_space=pltpu.SMEM)
        dma = pltpu.SemaphoreType.DMA
        lanes = 2 * dh
        return pl.pallas_call(
            functools.partial(layer_kernel, S, T, H, dh),
            out_shape=jax.ShapeDtypeStruct((R, D), bf16),
            in_specs=[vmem, vmem, vmem, vmem, vmem, smem, vmem, vmem],
            out_specs=vmem,
            scratch_shapes=[
                pltpu.VMEM((B, D), bf16),
                pltpu.VMEM((wo.shape[0] * T, D), bf16),
                pltpu.VMEM((H, B, lanes), bf16),
                pltpu.VMEM((H, half, lanes), bf16),
                pltpu.VMEM((S, B, lanes), bf16),
                pltpu.VMEM((H, half, lanes), bf16),
                pltpu.VMEM((2, half, lanes), bf16),
                pltpu.VMEM((B, half), bf16),
                pltpu.VMEM((2, half, lanes), f32),
                pltpu.VMEM((2, half, lanes), f32),
                pltpu.VMEM((H, T, R // 2, lanes), bf16),
                pltpu.VMEM((T * H, R // 2, lanes), bf16),
                pltpu.VMEM((R, T * H * dh), bf16),
                dma((T,)),
                dma((T,)),
                dma((T,)),
                dma((T,)),
                dma((H,)),
                dma((H * (G - 1),)),
                dma((S,)),
                dma((H,)),
                dma((H,)),
                dma((H * T,)),
                dma((T * H,)),
            ],
            compiler_params=pltpu.CompilerParams(has_side_effects=True, vmem_limit_bytes=50 * 2**20),
        )(act, gain_in.reshape(1, D), wq, wk, wv, off, wo, gain_out.reshape(1, D))

    in_specs = (
        P(("sp", "tp"), None),
        P(),
        P(None, "tp"),
        P(None, "tp"),
        P(None, "tp"),
        P("tp"),
        P("tp", None),
        P(),
    )
    out_specs = P(("sp", "tp"), None)
    return jax.shard_map(local, mesh=mesh, in_specs=in_specs, out_specs=out_specs, check_vma=False)
```

```python
import functools

import jax
import jax.numpy as jnp
from jax import lax
from jax.experimental import pallas as pl
from jax.experimental.pallas import tpu as pltpu
from jax.sharding import PartitionSpec as P

epsilon = 1e-06
log2e = 1.4426950408889634
MESH = pl.DeviceIdType.MESH
f32 = jnp.float32
bf16 = jnp.bfloat16


def scaled_rows(widened, row_gain):
    spread = jnp.mean(widened * widened, axis=-1, keepdims=True)
    return (widened * lax.rsqrt(spread + epsilon) * row_gain).astype(bf16)


def layer_kernel(
    S,
    T,
    H,
    dh,
    act,
    gain_in,
    wq_hbm,
    wk_hbm,
    wv_hbm,
    off,
    wo_hbm,
    gain_out,
    out,
    wq,
    wk,
    wv,
    xg,
    wg,
    kvs,
    qs,
    kv,
    qr,
    qpad,
    tri,
    acc,
    carry,
    obuf,
    orecv,
    att,
    x_send,
    x_recv,
    w_send,
    w_recv,
    kv_send,
    kv_relay,
    kv_recv,
    q_send,
    q_recv,
    o_send,
    o_recv,
    load,
):
    G = S // H
    R = act.shape[0]
    B = R * T
    half = B // 2
    rows = wo_hbm.shape[0]
    s = lax.axis_index("sp")
    t = lax.axis_index("tp")
    h, g = s // G, s % G
    y, c = t // 2, t % 2
    partner = y * 2 + 1 - c
    Y = T // 2

    def owner(group):
        turn = s % (2 * G) if group is None else None
        return jnp.where(turn < G, turn, 2 * G - 1 - turn)

    gq = owner(None)

    def block_of(k):
        return k * G + (g if k % 2 == 0 else G - 1 - g)

    def remote(src, dst, send, recv, dev):
        return pltpu.make_async_remote_copy(
            src_ref=src, dst_ref=dst, send_sem=send, recv_sem=recv, device_id=dev, device_id_type=MESH
        )

    started = []

    def go(copy):
        copy.start()
        started.append(copy)
        return copy

    def xrow(index):
        return xg.at[pl.ds(pl.multiple_of(index * R, R), R)]

    def wrow(index):
        return wg.at[pl.ds(pl.multiple_of(index * rows, rows), rows)]

    def x_copy(index, slot, dev):
        return remote(xrow(index), xrow(index), x_send.at[slot], x_recv.at[index], (s, dev))

    def w_copy(src, index, slot, dev):
        return remote(src, wrow(index), w_send.at[slot], w_recv.at[index], (s, dev))

    barrier = pltpu.get_barrier_semaphore()
    for d in range(1, S * T):
        other = (s * T + t + d) % (S * T)
        pl.semaphore_signal(barrier, inc=1, device_id=(other // T, other % T), device_id_type=MESH)
    loads = [
        pltpu.make_async_copy(wk_hbm, wk, load.at[0]),
        pltpu.make_async_copy(wv_hbm, wv, load.at[1]),
        pltpu.make_async_copy(wq_hbm, wq, load.at[2]),
        pltpu.make_async_copy(wo_hbm, wrow(t), load.at[3]),
    ]
    for copy in loads:
        copy.start()

    xg[pl.ds(pl.multiple_of(t * R, R), R)] = scaled_rows(act[...].astype(f32), gain_in[...])
    pl.semaphore_wait(barrier, S * T - 1)
    for e in range(1, Y):
        go(x_copy(t, e, ((y + e) % Y) * 2 + c))
    go(x_copy(t, 0, partner))
    high = lax.broadcasted_iota(jnp.int32, (B, half), 0)
    low = lax.broadcasted_iota(jnp.int32, (B, half), 1)
    tri[...] = (high > low).astype(f32).astype(bf16)
    for e in range(1, Y):
        came = ((y + e) % Y) * 2 + c
        x_copy(came, 0, partner).wait_recv()
        go(x_copy(came, Y + e - 1, partner))
    for copy in loads:
        copy.wait()
    for e in range(1, Y):
        go(w_copy(wrow(t), t, e, ((y + e) % Y) * 2 + c))
    x_copy(partner, 0, partner).wait_recv()
    for e in range(1, Y):
        x_copy(((y + e) % Y) * 2 + 1 - c, 0, partner).wait_recv()

    rows_all = xg[...]
    keys = jnp.dot(rows_all, wk[...], preferred_element_type=f32).astype(bf16)
    values = jnp.dot(rows_all, wv[...], preferred_element_type=f32).astype(bf16)
    for i in range(H):
        cols = slice(i * dh, (i + 1) * dh)
        kvs[i] = jnp.concatenate([keys[:, cols], values[:, cols]], axis=1)
    for d in range(1, H):
        hd = (h + d) % H
        go(remote(kvs.at[hd], kv.at[s], kv_send.at[d], kv_recv.at[s], (hd * G + g, t)))
    for e in range(1, G):
        remote(
            kvs.at[h], kv.at[s], kv_relay.at[h * (G - 1) + e - 1], kv_recv.at[s], (h * G + (g + e) % G, t)
        ).start()
    kv[s] = kvs[h]
    queries = jnp.dot(rows_all, wq[...], preferred_element_type=f32).astype(bf16)
    for i in range(H):
        cols = slice(i * dh, (i + 1) * dh)
        qs[i] = jnp.concatenate([queries[:half, cols], queries[half:, cols]], axis=1)
    for d in range(1, H):
        hd = (h + d) % H
        go(remote(qs.at[hd], qr.at[s // G], q_send.at[d], q_recv.at[s // G], (hd * G + gq, t)))

    own_q = remote(qs.at[h], qr.at[s // G], q_send.at[0], q_recv.at[s // G], (h * G + gq, t))

    @pl.when(gq != g)
    def _():
        own_q.start()

    @pl.when(gq == g)
    def _():
        qr[s // G] = qs[h]

    def kv_wait(j):
        remote(kvs.at[0], kv.at[j], kv_send.at[0], kv_recv.at[j], (s, t)).wait_recv()

    def relays(k):
        j = k * G + g
        return [
            remote(
                kv.at[j], kv.at[j], kv_relay.at[k * (G - 1) + e - 1], kv_recv.at[j], (h * G + (g + e) % G, t)
            )
            for e in range(1, G)
        ]

    def relay(k):
        @pl.when(k != h)
        def _():
            kv_wait(k * G + g)
            for copy in relays(k):
                copy.start()

    offset = off[h] * log2e
    factor = dh ** (-0.5) * log2e

    def piece(i, block, width, causal):
        key_tile = kv[block, :width]
        z = lax.dot_general(qpad[i], key_tile, (((1,), (1,)), ((), ())), preferred_element_type=f32)
        z = z * factor + offset
        keep = jnp.maximum(jnp.log2(1.0 + jnp.exp2(jnp.minimum(z, 100.0))), z)
        if causal:
            query_pos = i * half + lax.broadcasted_iota(jnp.int32, (half, width), 0)
            earlier = lax.broadcasted_iota(jnp.int32, (half, width), 1) < query_pos
            lost = jnp.where(earlier, keep, 0.0)
        else:
            lost = keep
        lost_b = lost.astype(bf16)
        first = jnp.dot(lost_b, tri[:width], preferred_element_type=f32)
        after = first
        if width > half:
            last = jnp.dot(lost_b[:, half:], tri[:half], preferred_element_type=f32)
            after = jnp.concatenate([first, last], axis=1)
        weight = jnp.exp2(z - keep - after)
        if causal:
            weight = jnp.where(earlier, weight, 0.0)
        part = jnp.dot(weight.astype(bf16), key_tile, preferred_element_type=f32)
        total = first[:, :1] + lost[:, :1]
        if causal:
            acc[i] = part
            carry[i] = jnp.broadcast_to(total, carry.shape[1:])
        else:
            before = carry[i]
            acc[i] += jnp.exp2(-before) * part
            carry[i] = before + total

    relay(0)
    for k in range(H):
        b = block_of(k)
        if k + 1 < H:
            relay(k + 1)
        for e in range(1, G):
            kv_wait(k * G + (g + e) % G)

        @pl.when(b != s)
        def _():
            remote(qs.at[0], qr.at[k], q_send.at[0], q_recv.at[k], (s, t)).wait_recv()

        packed = qr[k]
        blank = jnp.zeros((half, dh), bf16)
        qpad[0] = jnp.concatenate([packed[:, :dh], blank], axis=1)
        qpad[1] = jnp.concatenate([packed[:, dh:], blank], axis=1)
        piece(0, b, half, True)
        piece(1, b, B, True)

        def more(step, unused):
            piece(0, b - 1 - step, B, False)
            piece(1, b - 1 - step, B, False)
            return unused

        lax.fori_loop(0, b, more, 0)
        if k == H // 2 - 1:
            go(w_copy(wrow(t), t, 0, partner))
            for e in range(1, Y):
                came = ((y + e) % Y) * 2 + c
                w_copy(wrow(t), came, 0, partner).wait_recv()
                go(w_copy(wrow(came), came, Y + e - 1, partner))
        for r in range(T):
            chunk = acc[r * R // half, pl.ds(r * R % half, R)]
            obuf[k, r] = jnp.concatenate([chunk[: R // 2, dh:], chunk[R // 2 :, dh:]], axis=1).astype(bf16)
        for e in range(1, T):
            r = (t + e) % T
            go(remote(obuf.at[k, r], orecv.at[t * H + h], o_send.at[k * T + e], o_recv.at[t * H + h], (b, r)))
        own_o = remote(obuf.at[k, t], orecv.at[t * H + h], o_send.at[k * T], o_recv.at[t * H + h], (b, t))

        @pl.when(b != s)
        def _():
            own_o.start()

        @pl.when(b == s)
        def _():
            orecv[t * H + h] = obuf[k, t]

    w_copy(wrow(t), partner, 0, partner).wait_recv()
    for e in range(1, Y):
        w_copy(wrow(t), ((y + e) % Y) * 2 + 1 - c, 0, partner).wait_recv()

    for tt in range(T):
        for hh in range(H):

            @pl.when(jnp.logical_or(tt != t, hh * G + gq != s))
            def _():
                e = tt * H + hh
                remote(obuf.at[0, 0], orecv.at[e], o_send.at[0], o_recv.at[e], (s, t)).wait_recv()

    for p in range(T * H // 2):
        one, two = orecv[2 * p], orecv[2 * p + 1]
        cols = slice(2 * p * dh, (2 * p + 2) * dh)
        att[: R // 2, cols] = jnp.concatenate([one[:, :dh], two[:, :dh]], axis=1)
        att[R // 2 :, cols] = jnp.concatenate([one[:, dh:], two[:, dh:]], axis=1)
    projected = jnp.dot(att[...], wg[...], preferred_element_type=f32)
    out[...] = scaled_rows(projected, gain_out[...])

    for copy in started:
        copy.wait_send()
    for k in range(H):
        for copy in relays(k):
            copy.wait_send()

    @pl.when(gq != g)
    def _():
        own_q.wait_send()

    for k in range(H):
        b = block_of(k)

        @pl.when(b != s)
        def _():
            remote(obuf.at[k, t], orecv.at[t * H + h], o_send.at[k * T], o_recv.at[t * H + h], (b, t)).wait_send()


def solution(mesh):
    S, T = mesh.shape["sp"], mesh.shape["tp"]

    def local(act, gain_in, wq, wk, wv, off, wo, gain_out):
        R, D = act.shape
        H = off.shape[0]
        dh = wq.shape[1] // H
        G = S // H
        B = R * T
        half = B // 2
        vmem = pl.BlockSpec(memory_space=pltpu.VMEM)
        hbm = pl.BlockSpec(memory_space=pl.ANY)
        smem = pl.BlockSpec(memory_space=pltpu.SMEM)
        dma = pltpu.SemaphoreType.DMA
        lanes = 2 * dh
        return pl.pallas_call(
            functools.partial(layer_kernel, S, T, H, dh),
            out_shape=jax.ShapeDtypeStruct((R, D), bf16),
            in_specs=[vmem, vmem, hbm, hbm, hbm, smem, hbm, vmem],
            out_specs=vmem,
            scratch_shapes=[
                pltpu.VMEM(wq.shape, bf16),
                pltpu.VMEM(wk.shape, bf16),
                pltpu.VMEM(wv.shape, bf16),
                pltpu.VMEM((B, D), bf16),
                pltpu.VMEM((wo.shape[0] * T, D), bf16),
                pltpu.VMEM((H, B, lanes), bf16),
                pltpu.VMEM((H, half, lanes), bf16),
                pltpu.VMEM((S, B, lanes), bf16),
                pltpu.VMEM((H, half, lanes), bf16),
                pltpu.VMEM((2, half, lanes), bf16),
                pltpu.VMEM((B, half), bf16),
                pltpu.VMEM((2, half, lanes), f32),
                pltpu.VMEM((2, half, lanes), f32),
                pltpu.VMEM((H, T, R // 2, lanes), bf16),
                pltpu.VMEM((T * H, R // 2, lanes), bf16),
                pltpu.VMEM((R, T * H * dh), bf16),
                dma((T,)),
                dma((T,)),
                dma((T,)),
                dma((T,)),
                dma((H,)),
                dma((H * (G - 1),)),
                dma((S,)),
                dma((H,)),
                dma((H,)),
                dma((H * T,)),
                dma((T * H,)),
                dma((4,)),
            ],
            compiler_params=pltpu.CompilerParams(collective_id=0, has_side_effects=True, vmem_limit_bytes=50 * 2**20),
        )(act, gain_in.reshape(1, D), wq, wk, wv, off, wo, gain_out.reshape(1, D))

    in_specs = (
        P(("sp", "tp"), None),
        P(),
        P(None, "tp"),
        P(None, "tp"),
        P(None, "tp"),
        P("tp"),
        P("tp", None),
        P(),
    )
    out_specs = P(("sp", "tp"), None)
    return jax.shard_map(local, mesh=mesh, in_specs=in_specs, out_specs=out_specs, check_vma=False)
```
